32 devices in a mesh: ep: 8 (over z, x), tp: 4 (over y, core).
Axes of the slice: x: 2, y: 2, z: 4, core: 2. Of those that a mesh axis runs over, the one named last changes fastest.
Arguments:
- out_gate: bfloat16 [4096, 2048], P(('ep', 'tp')), may hold values from -6 to 6
- in_gate: bfloat16 [4096, 2048], P(('ep', 'tp')), may hold values from -6 to 6
- values: bfloat16 [4096, 2048], P(('ep', 'tp')), may hold values from -6 to 6
- conv_taps: float32 [3, 2048], replicated, may hold values from -4 to 4
- out_weight: bfloat16 [2048, 2048], P(None, 'tp'), may hold values from -0.125 to 0.125
- expert_input: bfloat16 [8192, 2048], P(('ep', 'tp')), may hold values from -6 to 6
- norm_gain: float32 [2048], replicated, may hold values from 0.1 to 1.9
- expert_ids: int32 [8192, 2], P(('ep', 'tp')), may hold values from 0 to 7, all different within a row; in each aligned block of 256 rows (0 to 255, 256 to 511, ...) at most 128 rows name the same one
- route_logits: float32 [8192, 2], P(('ep', 'tp')), may hold values from -8 to 8
- group_share: float32 [8192], P(('ep', 'tp')), may hold values from 0.3 to 1
- gate_weight: bfloat16 [8, 2048, 512], P('ep'), may hold values from -0.125 to 0.125
- up_weight: bfloat16 [8, 2048, 512], P('ep'), may hold values from -0.125 to 0.125
- down_weight: bfloat16 [8, 512, 2048], P('ep'), may hold values from -0.25 to 0.25
Outputs:
- mixer_out: bfloat16 [4096, 2048], P(('ep', 'tp'))
- expert_mix: bfloat16 [8192, 2048], P(('ep', 'tp'))
The draws below stay inside these ranges and needn't reach their ends.
Inputs may be any that keep to these rules, and one draw needn't show every extreme that they name: `expert_ids`: each row names 2 different experts. Within the rows of one device (aligned blocks of 256 rows) no expert is named by more than 128 rows, a bound that some block reaches.
All inputs are finite; a program needn't handle non-finite values.
Results may differ from the reference program's by a relative error of at most 0.0071.
Values may be sent and summed in bfloat16 or wider, within the bound.
A program may use at most 128 MiB of HBM per device.

```python
import math
import jax
import jax.numpy as jnp
import numpy as np
from jax import lax

D = 2048
F = 512
EXPERTS = 8
TOP = 2
CONV = 3
SEQS = 1
TOK_B = 256
TOKENS_A = 4096
TOKENS_B = 8192
CAP = 128
N_EP = 8
N_TP = 4


def levels(stream_key, dims, pieces, least, high):
    def one(axis_at, blocks):
        heights = jax.random.uniform(jax.random.fold_in(jax.random.fold_in(stream_key, 6), axis_at), (blocks,), jnp.float32, least / len(pieces), high / len(pieces))
        return jnp.repeat(jnp.exp(heights), dims[axis_at] // blocks).reshape((-1,) + (1,) * (len(dims) - axis_at - 1))

    loudness = one(*pieces[0])
    for cut in pieces[1:]:
        loudness = loudness * one(*cut)
    return loudness


def shared_out(stream_key, own, number, rows, amount, top, reach, slope):
    ranking = jax.random.permutation(stream_key, amount)
    heavy_load, common = shares(amount, rows * top, reach, slope, True), shares(amount, rows * top, reach, slope, False)
    places = jnp.arange(amount)

    def named(lengths, rotation):
        used = int((lengths > 0).sum())
        fixed = max(1, used // 4)
        shifted = fixed + (places - fixed + rotation * (used - fixed)) % max(1, amount - fixed)
        return jnp.zeros((amount,), jnp.int32).at[ranking[jnp.where(places < fixed, places, shifted)]].set(jnp.asarray(lengths, jnp.int32))

    lengths = jnp.where(number % 4 == 0, named(heavy_load, number // 4), named(common, number - number // 4 - 1))
    mixed = jax.random.permutation(jax.random.fold_in(own, 3), amount)
    giver, receiver = mixed[0:amount // 2 * 2:2], mixed[1:amount // 2 * 2:2]
    room = jnp.minimum(lengths[giver] - 1, reach - lengths[receiver]) // 2
    room = jnp.where((giver == ranking[0]) | (receiver == ranking[0]) | (lengths[receiver] == 0), 0, jnp.maximum(room, 0))
    shifted = jax.random.randint(jax.random.fold_in(own, 4), (amount // 2,), 0, 1 << 20) % (room + 1)
    lengths = lengths.at[giver].add(-shifted).at[receiver].add(shifted)
    items = jnp.searchsorted(jnp.cumsum(lengths), jnp.arange(rows * top), side="right").astype(jnp.int32)
    listing = items.reshape(top, rows).T
    listing = listing[jax.random.permutation(jax.random.fold_in(own, 1), rows)]
    rotation = jax.random.randint(jax.random.fold_in(own, 2), (rows, 1), 0, top)
    return jnp.take_along_axis(listing, (jnp.arange(top)[None, :] + rotation) % top, axis=1)


def shares(number_of, total, most, skew, full):
    loads = [(1 << 20) // math.isqrt(grade ** skew) + 1 for grade in range(1, number_of + 1)]
    largest = most if full else min(most, max(-(-total // number_of), total * loads[0] // sum(loads)))
    least = 1 if total - largest >= number_of - 1 else 0
    given, spare = [largest] + [least] * (number_of - 1), total - largest - least * (number_of - 1)
    while spare > 0:
        candidates = [i for i in range(1, number_of) if given[i] < largest] or [i for i in range(1, number_of) if given[i] < most]
        mass, left = sum([loads[i] for i in candidates]), spare
        for i in candidates:
            more = min(most - given[i], max(1, left * loads[i] // mass), spare)
            given[i] = given[i] + more
            spare = spare - more
    return np.array(given)


def scatter_about(key, dims, scale, limit, pieces=(), kind=jnp.bfloat16):
    factor_of = levels(key, dims, pieces, -0.22, 0.18) if pieces else 1.0
    values = jax.random.normal(key, dims, jnp.float32) * scale * factor_of
    return jnp.minimum(jnp.maximum(values, -limit), limit).astype(kind)


def setup_inputs(seed: int = 0) -> dict:
    streams_of = jax.random.split(jax.random.key(seed), 14)
    out_gate = scatter_about(streams_of[0], (TOKENS_A, D), 1.0, 6.0, ((0, 32),))
    in_gate = scatter_about(streams_of[1], (TOKENS_A, D), 1.0, 6.0, ((0, 32),))
    values = scatter_about(streams_of[2], (TOKENS_A, D), 1.0, 6.0, ((0, 32),))
    conv_taps = scatter_about(streams_of[3], (CONV, D), 0.6, 4.0, (), jnp.float32)
    out_weight = scatter_about(streams_of[4], (D, D), D ** -0.5, 0.125, ((1, 4),))
    expert_input = scatter_about(streams_of[5], (TOKENS_B, D), 1.0, 6.0, ((0, 32),))
    norm_gain = jnp.clip(1.0 + 0.18 * jax.random.normal(streams_of[6], (D,), jnp.float32), 0.1, 1.9)
    expert_ids_keys = jax.random.split(jax.random.fold_in(streams_of[7], 1), TOKENS_B // TOK_B)
    expert_ids_turns = jax.random.permutation(jax.random.fold_in(streams_of[7], 3), TOKENS_B // TOK_B)
    expert_ids = jax.vmap(lambda own, number: shared_out(jax.random.fold_in(streams_of[7], 2), own, number, TOK_B, EXPERTS, TOP, CAP, 2))(expert_ids_keys, expert_ids_turns).reshape((TOKENS_B, TOP))
    route_logits = scatter_about(streams_of[8], (TOKENS_B, TOP), 1.5, 8.0, ((0, 32),), jnp.float32)
    group_share = jnp.clip(0.3 + 0.7 * jax.random.uniform(streams_of[9], (TOKENS_B,), jnp.float32) ** levels(streams_of[9], (TOKENS_B,), ((0, 32),), -0.2, 0.2), 0.3, 1.0)
    gate_weight = scatter_about(streams_of[10], (EXPERTS, D, F), D ** -0.5, 0.125, ((0, 8),))
    up_weight = scatter_about(streams_of[11], (EXPERTS, D, F), D ** -0.5, 0.125, ((0, 8),))
    down_weight = scatter_about(streams_of[12], (EXPERTS, F, D), F ** -0.5, 0.25, ((0, 8),))
    return {"out_gate": out_gate, "in_gate": in_gate, "values": values, "conv_taps": conv_taps, "out_weight": out_weight, "expert_input": expert_input, "norm_gain": norm_gain, "expert_ids": expert_ids, "route_logits": route_logits, "group_share": group_share, "gate_weight": gate_weight, "up_weight": up_weight, "down_weight": down_weight}


norm_eps = 1e-05

def reference(out_gate, in_gate, values, conv_taps, out_weight, expert_input, norm_gain, expert_ids, route_logits, group_share, gate_weight, up_weight, down_weight):
    gated = (in_gate.astype(jnp.float32) * values.astype(jnp.float32)).astype(jnp.bfloat16)
    per_seq = gated.reshape(SEQS, -1, D).astype(jnp.float32)
    length = per_seq.shape[1]
    padded = jnp.pad(per_seq, ((0, 0), (CONV - 1, 0), (0, 0)))
    filtered = jnp.zeros_like(per_seq)
    for index in range(CONV):
        filtered = filtered + padded[:, index:index + length] * conv_taps[index]
    mixed_rows = (out_gate.astype(jnp.float32) * filtered.reshape(-1, D)).astype(jnp.bfloat16)
    mixer_out = jnp.dot(mixed_rows, out_weight, preferred_element_type=jnp.float32).astype(jnp.bfloat16)
    inputs = expert_input.astype(jnp.float32)
    scale = lax.rsqrt(lax.optimization_barrier(jnp.mean(inputs * inputs, axis=-1, keepdims=True)) + norm_eps)
    normed = (inputs * scale * norm_gain).astype(jnp.bfloat16)
    total = TOKENS_B * TOP
    flat_ids = expert_ids.reshape(-1).astype(jnp.int32)
    order = jnp.argsort(flat_ids, stable=True).astype(jnp.int32)
    counts = jax.ops.segment_sum(jnp.ones((total,), jnp.int32), flat_ids, EXPERTS).astype(jnp.int32)
    starts = (jnp.cumsum(counts) - counts).astype(jnp.int32)
    bound = N_EP * N_TP * CAP
    steps_in = jnp.arange(bound, dtype=jnp.int32)

    def per_expert(stored, expert):
        places = starts[expert] + steps_in
        valid = steps_in < counts[expert]
        entry = order[jnp.minimum(places, total - 1)]
        rows = normed[entry // TOP]
        gate = jnp.dot(rows, gate_weight[expert], preferred_element_type=jnp.float32)
        upper = jnp.dot(rows, up_weight[expert], preferred_element_type=jnp.float32)
        hidden = (jax.nn.silu(gate) * upper).astype(jnp.bfloat16)
        result = jnp.dot(hidden, down_weight[expert], preferred_element_type=jnp.float32).astype(jnp.bfloat16)
        target = jnp.where(valid, entry, total).astype(jnp.int32)
        return (stored.at[target].set(result, mode='drop'), None)
    stored = jnp.zeros((total, D), jnp.bfloat16)
    stored, _ = lax.scan(per_expert, stored, jnp.arange(EXPERTS, dtype=jnp.int32))
    expert_out = stored.reshape(TOKENS_B, TOP, D).astype(jnp.float32)
    margin = route_logits[:, 0] - route_logits[:, 1]
    route_weight = group_share[:, None] * jnp.stack([jax.nn.sigmoid(margin), jax.nn.sigmoid(-margin)], axis=1)
    expert_mix = lax.optimization_barrier(jnp.sum(expert_out * route_weight[:, :, None], axis=1)).astype(jnp.bfloat16)
    return (mixer_out, expert_mix)
```

```python
import functools

import jax
import jax.numpy as jnp
from jax import lax
from jax.experimental import pallas as pl
from jax.experimental.pallas import tpu as pltpu
from jax.sharding import PartitionSpec as P

SEQS = 1


norm_eps = 1e-05


def passed_along(value, axis, by):
    length = lax.axis_size(axis)
    pairs = [(i, i + by) for i in range(length) if 0 <= i + by < length]
    return lax.ppermute(value, axis, pairs)


def local(
    out_gate,
    in_gate,
    values,
    conv_taps,
    out_weight,
    expert_input,
    norm_gain,
    expert_ids,
    route_logits,
    group_share,
    gate_weight,
    up_weight,
    down_weight,
):
    rows_mix, width = out_gate.shape
    extent = conv_taps.shape[0] - 1
    gated = (in_gate.astype(jnp.float32) * values.astype(jnp.float32)).astype(jnp.bfloat16)
    before = passed_along(gated[rows_mix - extent :], ("ep", "tp"), 1)
    extended = jnp.concatenate([before, gated], axis=0)
    devices = lax.axis_size("ep") * lax.axis_size("tp")
    seq_len = devices * rows_mix // SEQS
    position = lax.axis_index(("ep", "tp")) * rows_mix + jnp.arange(rows_mix, dtype=jnp.int32)
    offset = position % seq_len
    filtered = jnp.zeros((rows_mix, width), jnp.float32)
    for delays in range(extent + 1):
        lagged = extended[extent - delays : extent - delays + rows_mix].astype(jnp.float32)
        if delays > 0:
            lagged = jnp.where((offset >= delays)[:, None], lagged, 0.0)
        filtered = filtered + conv_taps[extent - delays] * lagged
    mixed_rows = (out_gate.astype(jnp.float32) * filtered).astype(jnp.bfloat16)
    mixer_out = jnp.dot(
        mixed_rows,
        lax.all_gather(out_weight, "tp", axis=1, tiled=True),
        preferred_element_type=jnp.float32,
    ).astype(jnp.bfloat16)
    tokens, width = expert_input.shape
    chosen = expert_ids.shape[1]
    experts = lax.axis_size("ep") * gate_weight.shape[0]
    capacity = 2 * tokens * chosen // experts
    inputs = expert_input.astype(jnp.float32)
    scale = lax.rsqrt(jnp.mean(inputs * inputs, axis=-1, keepdims=True) + norm_eps)
    normed = (inputs * scale * norm_gain).astype(jnp.bfloat16)
    flat_ids = expert_ids.reshape(-1)
    entries = flat_ids.shape[0]
    one_hot = (flat_ids[:, None] == jnp.arange(experts, dtype=jnp.int32)[None, :]).astype(jnp.int32)
    earlier = jnp.cumsum(one_hot, axis=0) - one_hot
    slots = jnp.sum(earlier * one_hot, axis=1)
    target = flat_ids * capacity + slots
    owner = (
        jnp.zeros((experts * capacity,), jnp.int32)
        .at[target]
        .set(jnp.arange(entries, dtype=jnp.int32) // chosen)
    )
    filled = jnp.zeros((experts * capacity,), jnp.bfloat16).at[target].set(1.0)
    outgoing = (normed[owner] * filled[:, None]).reshape(experts, capacity, width)
    arrived = lax.all_to_all(outgoing, "ep", split_axis=0, concat_axis=0, tiled=True)
    rows = arrived.reshape(-1, width)
    gate = jnp.dot(rows, gate_weight[0], preferred_element_type=jnp.float32)
    upper = jnp.dot(rows, up_weight[0], preferred_element_type=jnp.float32)
    hidden = (jax.nn.silu(gate) * upper).astype(jnp.bfloat16)
    result = jnp.dot(hidden, down_weight[0], preferred_element_type=jnp.float32).astype(
        jnp.bfloat16
    )
    results = result.reshape(arrived.shape)
    returned = lax.all_to_all(results, "ep", split_axis=0, concat_axis=0, tiled=True)
    picked = returned.reshape(experts * capacity, width)[target].reshape(tokens, chosen, width)
    margin = route_logits[:, 0] - route_logits[:, 1]
    route_weight = group_share[:, None] * jnp.stack(
        [jax.nn.sigmoid(margin), jax.nn.sigmoid(-margin)], axis=1
    )
    expert_mix = jnp.sum(picked.astype(jnp.float32) * route_weight[:, :, None], axis=1).astype(
        jnp.bfloat16
    )
    return (mixer_out, expert_mix)


MESH = pl.DeviceIdType.MESH
PAIR = 2
HALVES = 2
PARTS = 4
SUBS = 8
LAG = 3
HALO = 16


def fits(mesh):
    return mesh.shape["tp"] == PAIR * PAIR and mesh.shape["ep"] == 2 * PAIR * PAIR


def kernel(
    line,
    tok_in,
    gain,
    ids,
    logits,
    gshare,
    og_in,
    ig_in,
    val_in,
    taps,
    ow_in,
    gate_in,
    up_in,
    down_in,
    mixer_ref,
    mix_ref,
    tok,
    share,
    from_n,
    from_f,
    part,
    acc,
    packed,
    packed_in,
    gate,
    up,
    down,
    ow,
    local_sem,
    tok_f,
    tok_n,
    tok_got,
    share_f,
    share_n,
    share_got,
    n_got,
    f_got,
    part_sent,
    packed_sent,
    packed_got,
    x_sent,
    x_got,
    y_sent,
    y_got,
    c_sent,
    c_got,
    d_sent,
    d_got,
    m_sent,
    m_got,
    raw,
    og,
    ig,
    val,
    halo_out,
    halo,
    ext,
    mixed,
    mix_sem,
    halo_sent,
    halo_got,
):
    ep, tp = lax.axis_index("ep"), lax.axis_index("tp")
    z = ep // PAIR
    lanes = PAIR * PAIR
    pieces = 3 * SUBS
    x_ep = ep + 1 - 2 * (ep % PAIR)
    over_x = {"ep": x_ep, "tp": tp}
    over_y = {"ep": ep, "tp": (tp + PAIR) % lanes}
    over_c = {"ep": ep, "tp": tp + 1 - 2 * (tp % PAIR)}
    y_tp = (tp + PAIR) % lanes

    half = line // 2
    lower = z < half
    step = jnp.where(lower, 1, -1)
    base = jnp.where(lower, 0, line - 1)
    q = jnp.where(lower, z, line - 1 - z)
    outer, inner = q == 0, q == 1
    toward = {"ep": ep + PAIR * step, "tp": tp}
    back = {"ep": ep - PAIR * step, "tp": tp}

    tokens = tok.shape[1]
    rows = tokens // HALVES
    small = tokens // PARTS

    def blk(m):
        return base + step * m

    def remote(src, dst, sent, got, device):
        return pltpu.make_async_remote_copy(
            src_ref=src, dst_ref=dst, send_sem=sent, recv_sem=got,
            device_id=device, device_id_type=MESH,
        )

    def span(h):
        return pl.ds(pl.multiple_of(h * rows, rows), rows)

    def short(p):
        return pl.ds(pl.multiple_of(p * small, small), small)

    def tok_copy(m, h, sent, device):
        piece = tok.at[blk(m), span(h)]
        return remote(piece, piece, sent.at[m, h], tok_got.at[blk(m), h], device)

    def share_copy(m, sent, device):
        piece = share.at[blk(m)]
        return remote(piece, piece, sent.at[m], share_got.at[blk(m)], device)

    def send_f(m, h):
        if h == 0:
            share_copy(m, share_f, toward).start()
        tok_copy(m, h, tok_f, toward).start()

    def send_n(m, h):
        if h == 0:
            share_copy(m, share_n, back).start()
        tok_copy(m, h, tok_n, back).start()

    def got_tok(m, h):
        if h == 0:
            share_copy(m, share_f, toward).wait_recv()
        tok_copy(m, h, tok_f, toward).wait_recv()

    lin = ep * lanes + tp
    devices = line * PAIR * lanes
    has_next, has_prev = lin < devices - 1, lin > 0
    to_next = {"ep": (lin + 1) // lanes, "tp": (lin + 1) % lanes}
    to_prev = {"ep": (lin - 1) // lanes, "tp": (lin + lanes - 1) % lanes}

    first = [
        pltpu.make_async_copy(tok_in.at[span(h)], raw.at[span(h)], local_sem.at[h])
        for h in range(HALVES)
    ]
    for load in first:
        load.start()
    mix_loads = [
        pltpu.make_async_copy(src, dst, mix_sem.at[i])
        for i, (src, dst) in enumerate(((ig_in, ig), (val_in, val), (og_in, og)))
    ]
    for load in mix_loads:
        load.start()
    loads = [
        pltpu.make_async_copy(gate_in, gate.at[0], local_sem.at[2]),
        pltpu.make_async_copy(up_in, up.at[0], local_sem.at[3]),
        pltpu.make_async_copy(down_in, down.at[0], local_sem.at[4]),
        pltpu.make_async_copy(ow_in, ow.at[tp], local_sem.at[5]),
    ]

    barrier = pltpu.get_barrier_semaphore()
    for device in (over_x, over_y, over_c, toward):
        pl.semaphore_signal(barrier, inc=1, device_id=device, device_id_type=MESH)
    for there, device in ((inner, back), (has_next, to_next), (has_prev, to_prev)):

        @pl.when(there)
        def _():
            pl.semaphore_signal(barrier, inc=1, device_id=device, device_id_type=MESH)

    def edge(cond):
        return cond.astype(jnp.int32)

    pl.semaphore_wait(barrier, 4 + edge(inner) + edge(has_next) + edge(has_prev))

    mats = ((gate_in, gate), (up_in, up), (down_in, down))

    def piece(mat, sub, own):
        n = mats[mat][0].shape[0] // lanes
        k = n // SUBS
        return pl.ds(pl.multiple_of(own * n + sub * k, k), k)

    def x_copy(mat, sub):
        src, dst = mats[mat]
        return remote(
            src.at[piece(mat, sub, tp)], dst.at[1, piece(mat, sub, tp)],
            x_sent.at[mat, sub], x_got.at[mat, sub], over_x,
        )

    def spread(mat, sub, own, sent, got, device):
        ref = mats[mat][1].at[1, piece(mat, sub, own)]
        return remote(ref, ref, sent.at[mat, sub], got.at[mat, sub], device)

    for mat in range(3):
        for sub in range(SUBS):
            x_copy(mat, sub).start()

    depth = ow_in.shape[0]
    cut = depth // (4 * lanes)

    def m_own():
        return remote(ow_in, ow.at[tp], m_sent.at[0], m_got.at[0], over_c)

    def m_part(i):
        r = pl.ds(0, cut) if i == 0 else pl.ds(cut, depth - cut)
        return remote(ow_in.at[r], ow.at[tp, r], m_sent.at[1 + i], m_got.at[1 + i], over_y)

    def m_far():
        return remote(ow.at[y_tp], ow.at[y_tp], m_sent.at[3], m_got.at[3], over_c)

    m_part(0).start()

    def norm(h):
        first[h].wait()
        r = raw[span(h)].astype(jnp.float32)
        scale = lax.rsqrt(jnp.mean(r * r, axis=-1, keepdims=True) + norm_eps)
        tok[z, span(h)] = (r * scale * gain[...]).astype(jnp.bfloat16)

    norm(0)
    n_experts = share.shape[2]
    of = lax.broadcasted_iota(jnp.int32, (n_experts, rows), 0)
    for h in range(HALVES):
        cols = slice(h * rows, (h + 1) * rows)
        margin = logits[0:1, cols] - logits[1:2, cols]
        share[z, h] = gshare[:, cols] * (
            jnp.where(ids[0:1, cols] == of, 1.0 / (1.0 + jnp.exp(-margin)), 0.0)
            + jnp.where(ids[1:2, cols] == of, 1.0 / (1.0 + jnp.exp(margin)), 0.0)
        )

    @pl.when(outer)
    def _():
        send_f(0, 0)

    @pl.when(inner)
    def _():
        send_f(1, 0)
        send_n(1, 0)

    norm(1)
    mix_loads[0].wait()
    mix_loads[1].wait()
    n_mix = ig.shape[0]
    last = pl.ds(n_mix - HALO, HALO)
    halo_out[...] = (ig[last].astype(jnp.float32) * val[last].astype(jnp.float32)).astype(
        jnp.bfloat16
    )

    @pl.when(outer)
    def _():
        send_f(0, 1)

    @pl.when(inner)
    def _():
        send_n(1, 1)

    def halo_copy():
        return remote(halo_out, halo, halo_sent.at[0], halo_got.at[0], to_next)

    @pl.when(has_next)
    def _():
        halo_copy().start()

    for load in loads:
        load.start()

    sub_iota = lax.broadcasted_iota(jnp.int32, (rows, rows), 0)
    lane_iota = lax.broadcasted_iota(jnp.int32, (rows, rows), 1)
    eye = sub_iota == lane_iota

    def column(row):
        return jnp.sum(jnp.where(eye, row, 0.0), axis=1, keepdims=True)

    def of_expert(table, e):
        return jnp.sum(jnp.where(of == e, table, 0.0), axis=0, keepdims=True)

    held = (ep, x_ep)

    def expert(i, x):
        a = jnp.dot(x, gate[i], preferred_element_type=jnp.float32)
        c = jnp.dot(x, up[i], preferred_element_type=jnp.float32)
        hidden = (a / (1.0 + jnp.exp(-a)) * c).astype(jnp.bfloat16)
        return jnp.dot(hidden, down[i], preferred_element_type=jnp.float32)

    def dense(i, m, h):
        b = blk(m)
        return column(of_expert(share[b, h], held[i])) * expert(i, tok[b, span(h)])

    def own_unit(m, h):
        acc[m, span(h)] = dense(0, m, h)

    def slots_of(m, e):
        ahead = (sub_iota < lane_iota).astype(jnp.bfloat16)
        before = jnp.zeros((n_experts, 1), jnp.float32)
        found = []
        for h in range(HALVES):
            named = (share[blk(m), h] != 0.0).astype(jnp.float32)
            places = before + jnp.dot(
                named.astype(jnp.bfloat16), ahead, preferred_element_type=jnp.float32
            )
            before = before + jnp.sum(named, axis=1, keepdims=True)
            weight = of_expert(share[blk(m), h], e)
            found.append((of_expert(jnp.where(named > 0.0, places, -1.0), e), weight))
        return found

    def pack(i):
        b = blk(1)
        x, weight = None, None
        for h, (place, w) in enumerate(slots_of(1, held[i])):
            pick = place == sub_iota.astype(jnp.float32)
            term = jnp.dot(
                pick.astype(jnp.bfloat16), tok[b, span(h)], preferred_element_type=jnp.float32
            )
            w_term = jnp.sum(jnp.where(pick, w, 0.0), axis=1, keepdims=True)
            x = term if x is None else x + term
            weight = w_term if weight is None else weight + w_term
        packed[i] = (weight * expert(i, x.astype(jnp.bfloat16))).astype(jnp.bfloat16)

    def packed_copy(i):
        return remote(
            packed.at[i], packed_in.at[i], packed_sent.at[i], packed_got.at[i], toward
        )

    def unpack(i):
        packed_copy(i).wait_recv()
        for h, (place, _) in enumerate(slots_of(1, held[i] - PAIR * step)):
            spot = (column(place) == lane_iota.astype(jnp.float32)).astype(jnp.bfloat16)
            acc[1, span(h)] += jnp.dot(spot, packed_in[i], preferred_element_type=jnp.float32)

    def each(i, act):
        for mat in range(3):

            @pl.when(i // SUBS == mat)
            def _():
                act(mat, i % SUBS)

    def x_round(mat, sub):
        x_copy(mat, sub).wait_recv()
        spread(mat, sub, tp, y_sent, y_got, over_y).start()
        spread(mat, sub, tp, c_sent, c_got, over_c).start()

    def y_round(mat, sub):
        spread(mat, sub, tp, y_sent, y_got, over_y).wait_recv()
        spread(mat, sub, y_tp, d_sent, d_got, over_c).start()

    def gather_step(i, _):
        each(i, x_round)

        @pl.when(i == pieces - 1)
        def _():
            m_part(1).start()
            m_own().start()

        @pl.when(i >= LAG)
        def _():
            each(i - LAG, y_round)

        @pl.when(i == 0)
        def _():
            for load in loads:
                load.wait()

        @pl.when(inner & (i == SUBS - 1))
        def _():
            got_tok(0, 0)
            send_f(0, 0)
            got_tok(2, 0)

        @pl.when(inner & (i == 2 * SUBS - 1))
        def _():
            got_tok(0, 1)
            send_f(0, 1)
            send_f(1, 1)
            got_tok(3, 0)
            send_n(3, 0)

        @pl.when(inner & (i == 3 * SUBS - 1))
        def _():
            got_tok(3, 1)
            send_n(3, 1)
            send_n(2, 0)

        @pl.when(outer & (i == SUBS - 1))
        def _():
            got_tok(1, 0)

        @pl.when(outer & (i == 2 * SUBS - 1))
        def _():
            got_tok(1, 1)

        @pl.when(outer & (i == 3 * SUBS - 1))
        def _():
            got_tok(3, 0)

        r = i % SUBS
        s = (i // SUBS) * 2 + r // 2

        @pl.when(((r == 1) | (r == 3)) & (inner | (i < SUBS)))
        def _():
            m = jnp.where(s < 2, q, jnp.where(s == 3, 2, jnp.where(s == 4, 3, 0)))
            own_unit(m, jnp.where((s == 1) | (s == 5), 1, 0))

        @pl.when(outer & (i == 2 * SUBS))
        def _():
            pack(0)
            packed_copy(0).start()

        return 0

    lax.fori_loop(0, pieces, gather_step, 0)

    own_unit(3, jnp.where(inner, 1, 0))

    for i in range(pieces - LAG, pieces):
        y_round(i // SUBS, i % SUBS)
    for mat in range(3):
        for sub in range(SUBS):
            spread(mat, sub, tp, c_sent, c_got, over_c).wait_recv()
            spread(mat, sub, y_tp, d_sent, d_got, over_c).wait_recv()

    def ahead_copy(m, p):
        src, sent = part.at[m - 2, short(p)], part_sent.at[m - 2, p]
        return src, sent

    def outer_send(m, p):
        src, sent = ahead_copy(m, p)
        return remote(src, from_n.at[m - 2, short(p)], sent, n_got.at[m - 2, p], toward)

    def inner_send(m, p):
        src, sent = ahead_copy(m, p)
        there = line - 1 - m
        return remote(src, from_f.at[there, short(p)], sent, f_got.at[there, p], toward)

    def home_send(p):
        return remote(
            part.at[2, short(p)], from_f.at[0, short(p)], part_sent.at[2, p], f_got.at[0, p], back
        )

    def n_wait(m, p):
        outer_send(m, p).wait_recv()

    def f_wait(m, p):
        ref = from_f.at[m, short(p)]
        remote(ref, ref, part_sent.at[0, p], f_got.at[m, p], toward).wait_recv()

    def mix_conv():
        ext[pl.ds(8, n_mix)] = (
            (ig[...].astype(jnp.float32) * val[...].astype(jnp.float32))
            .astype(jnp.bfloat16)
            .astype(jnp.float32)
        )

        @pl.when(has_prev)
        def _():
            halo_copy().wait_recv()

        opens = lin % (devices // SEQS) == 0

        @pl.when(opens)
        def _():
            ext[pl.ds(0, 8)] = jnp.zeros((8, ext.shape[1]), jnp.float32)

        @pl.when(jnp.logical_not(opens))
        def _():
            ext[pl.ds(0, 8)] = halo[...].astype(jnp.float32)[HALO - 8 :]

        mix_loads[2].wait()
        n_taps = taps.shape[0]
        filtered = None
        for t in range(n_taps):
            term = taps[pl.ds(t, 1)] * ext[pl.ds(8 - n_taps + 1 + t, n_mix)]
            filtered = term if filtered is None else filtered + term
        mixed[...] = (og[...].astype(jnp.float32) * filtered).astype(jnp.bfloat16)

    def mix_out():
        for i in range(2):
            m_part(i).wait_recv()
        m_far().start()
        m_own().wait_recv()
        m_far().wait_recv()
        n = ow.shape[2]
        for p in range(lanes):
            mixer_ref[:, p * n : (p + 1) * n] = jnp.dot(
                mixed[...], ow[p], preferred_element_type=jnp.float32
            ).astype(jnp.bfloat16)

    def outer_step(g, _):
        m, h = jnp.where(g < 2, 3, 2), g % HALVES
        part[m - 2, span(h)] = (acc[m, span(h)] + dense(1, m, h)).astype(jnp.bfloat16)
        for k in range(PARTS // HALVES):
            outer_send(m, h * (PARTS // HALVES) + k).start()

        @pl.when(g == 0)
        def _():
            got_tok(3, 1)

        @pl.when(g == 1)
        def _():
            mix_conv()
            got_tok(2, 0)

        @pl.when(g == 2)
        def _():
            got_tok(2, 1)

        @pl.when(g < 3)
        def _():
            own_unit(jnp.where(g < 1, 3, 2), (g + 1) % HALVES)

        return 0

    def inner_step(s, _):
        @pl.when(s < 8)
        def _():
            m = jnp.where(
                s < 2, 3, jnp.where(s < 4, 0, jnp.where(s < 6, 2, 1))
            )
            acc[m, span(s % HALVES)] += dense(1, m, s % HALVES)

        @pl.when((s >= 2) & (s < 2 + 2 * PARTS))
        def _():
            n = s - 2
            m, p = jnp.where(n < PARTS, 3, 2), n % PARTS
            n_wait(m, p)
            part[m - 2, short(p)] = (
                acc[m, short(p)] + from_n[m - 2, short(p)].astype(jnp.float32)
            ).astype(jnp.bfloat16)
            inner_send(m, p).start()

        @pl.when(s == 3)
        def _():
            got_tok(2, 1)
            send_n(2, 1)

        @pl.when(s == 2 + 2 * PARTS)
        def _():
            mix_out()

        @pl.when(s >= 3)
        def _():
            f = s - 3
            m, p = f // PARTS, f % PARTS
            f_wait(m, p)
            acc[m, short(p)] += from_f[m, short(p)].astype(jnp.float32)

            @pl.when(m == 0)
            def _():
                part[2, short(p)] = acc[0, short(p)].astype(jnp.bfloat16)
                home_send(p).start()

        @pl.when(s == 4)
        def _():
            own_unit(2, 1)

        @pl.when(s == 5)
        def _():
            unpack(0)

        @pl.when(s == 6)
        def _():
            mix_conv()

        return 0

    @pl.when(outer)
    def _():
        lax.fori_loop(0, 4, outer_step, 0)
        pack(1)
        packed_copy(1).start()

        def own_rest(h, _):
            acc[0, span(h)] += dense(1, 0, h)
            return 0

        lax.fori_loop(0, HALVES, own_rest, 0)

        def take(p, _):
            @pl.when(p == PARTS - 1)
            def _():
                mix_out()

            f_wait(0, p)
            mix_ref[short(p)] = (
                acc[0, short(p)] + from_f[0, short(p)].astype(jnp.float32)
            ).astype(jnp.bfloat16)
            return 0

        lax.fori_loop(0, PARTS, take, 0)

    @pl.when(inner)
    def _():
        lax.fori_loop(0, 3 + 2 * PARTS, inner_step, 0)
        unpack(1)
        mix_ref[...] = acc[1].astype(jnp.bfloat16)

    def sent_tok(m, copies, device, shares):
        share_copy(m, shares, device).wait_send()
        for h in range(HALVES):
            tok_copy(m, h, copies, device).wait_send()

    sent_tok(0, tok_f, toward, share_f)

    @pl.when(inner)
    def _():
        sent_tok(1, tok_f, toward, share_f)
        for m in (1, 2, 3):
            sent_tok(m, tok_n, back, share_n)
        for p in range(PARTS):
            home_send(p).wait_send()

    for m in (2, 3):
        for p in range(PARTS):
            outer_send(m, p).wait_send()

    @pl.when(outer)
    def _():
        for i in range(PAIR):
            packed_copy(i).wait_send()

    @pl.when(has_next)
    def _():
        halo_copy().wait_send()

    for mat in range(3):
        for sub in range(SUBS):
            x_copy(mat, sub).wait_send()
            spread(mat, sub, tp, y_sent, y_got, over_y).wait_send()
            spread(mat, sub, tp, c_sent, c_got, over_c).wait_send()
            spread(mat, sub, y_tp, d_sent, d_got, over_c).wait_send()
    m_own().wait_send()
    for i in range(2):
        m_part(i).wait_send()
    m_far().wait_send()


def paired(
    out_gate,
    in_gate,
    values,
    conv_taps,
    out_weight,
    expert_input,
    norm_gain,
    expert_ids,
    route_logits,
    group_share,
    gate_weight,
    up_weight,
    down_weight,
):
    tokens, width = expert_input.shape
    experts = lax.axis_size("ep") * gate_weight.shape[0]
    rows_mix, width = out_gate.shape
    line = lax.axis_size("ep") // PAIR
    lanes = lax.axis_size("tp")
    hidden = gate_weight.shape[2]
    packed_rows = 2 * tokens * expert_ids.shape[1] // experts
    dma = pltpu.SemaphoreType.DMA
    bf16, f32 = jnp.bfloat16, jnp.float32
    vmem = pl.BlockSpec(memory_space=pltpu.VMEM)
    hbm = pl.BlockSpec(memory_space=pl.ANY)
    return pl.pallas_call(
        functools.partial(kernel, line),
        out_shape=(
            jax.ShapeDtypeStruct((rows_mix, width), bf16),
            jax.ShapeDtypeStruct((tokens, width), bf16),
        ),
        in_specs=[hbm, vmem, vmem, vmem, vmem, hbm, hbm, hbm, vmem, hbm, hbm, hbm, hbm],
        out_specs=(vmem, vmem),
        scratch_shapes=[
            pltpu.VMEM((line, tokens, width), bf16),
            pltpu.VMEM((line, HALVES, experts, tokens // HALVES), f32),
            pltpu.VMEM((2, tokens, width), bf16),
            pltpu.VMEM((2, tokens, width), bf16),
            pltpu.VMEM((3, tokens, width), bf16),
            pltpu.VMEM((line, tokens, width), f32),
            pltpu.VMEM((PAIR, packed_rows, width), bf16),
            pltpu.VMEM((PAIR, packed_rows, width), bf16),
            pltpu.VMEM((PAIR, width, hidden), bf16),
            pltpu.VMEM((PAIR, width, hidden), bf16),
            pltpu.VMEM((PAIR, hidden, width), bf16),
            pltpu.VMEM((lanes,) + out_weight.shape, bf16),
            dma((6,)),
            dma((line, HALVES)),
            dma((line, HALVES)),
            dma((line, HALVES)),
            dma((line,)),
            dma((line,)),
            dma((line,)),
            dma((2, PARTS)),
            dma((2, PARTS)),
            dma((3, PARTS)),
            dma((PAIR,)),
            dma((PAIR,)),
            dma((3, SUBS)),
            dma((3, SUBS)),
            dma((3, SUBS)),
            dma((3, SUBS)),
            dma((3, SUBS)),
            dma((3, SUBS)),
            dma((3, SUBS)),
            dma((3, SUBS)),
            dma((4,)),
            dma((4,)),
            pltpu.VMEM((tokens, width), bf16),
            pltpu.VMEM((rows_mix, width), bf16),
            pltpu.VMEM((rows_mix, width), bf16),
            pltpu.VMEM((rows_mix, width), bf16),
            pltpu.VMEM((HALO, width), bf16),
            pltpu.VMEM((HALO, width), bf16),
            pltpu.VMEM((rows_mix + 8, width), f32),
            pltpu.VMEM((rows_mix, width), bf16),
            dma((3,)),
            dma((1,)),
            dma((1,)),
        ],
        compiler_params=pltpu.CompilerParams(
            collective_id=0, has_side_effects=True, vmem_limit_bytes=60 * 1024 * 1024
        ),
    )(
        expert_input,
        norm_gain[None],
        expert_ids.T,
        route_logits.T,
        group_share[None],
        out_gate,
        in_gate,
        values,
        conv_taps,
        out_weight,
        gate_weight[0],
        up_weight[0],
        down_weight[0],
    )


def solution(mesh):
    body = paired if fits(mesh) else local
    return jax.shard_map(
        body,
        mesh=mesh,
        in_specs=(
            P(("ep", "tp"), None),
            P(("ep", "tp"), None),
            P(("ep", "tp"), None),
            P(),
            P(None, "tp"),
            P(("ep", "tp"), None),
            P(),
            P(("ep", "tp"), None),
            P(("ep", "tp"), None),
            P(("ep", "tp")),
            P("ep", None, None),
            P("ep", None, None),
            P("ep", None, None),
        ),
        out_specs=(P(("ep", "tp"), None), P(("ep", "tp"), None)),
        check_vma=False,
    )
```
